512 devices in a mesh: sp: 16 (over z), fs: 4 (over y), tp: 8 (over x, core).
Axes of the slice: x: 4, y: 4, z: 16, core: 2. Of those that a mesh axis runs over, the one named last changes fastest.
Arguments:
- activations: bfloat16 [8192, 4096], P(('fs', 'sp'), 'tp'), parts along dimension 0, may hold values from -6 to 6
- input_norm_gain: float32 [4096], replicated, may hold values from 0.1 to 1.9
- window_query_weight: bfloat16 [4096, 2048], P('sp', 'tp'), may hold values from -0.09375 to 0.09375
- window_key_weight: bfloat16 [4096, 512], P('sp', 'tp'), may hold values from -0.09375 to 0.09375
- window_value_weight: bfloat16 [4096, 512], P('sp', 'tp'), may hold values from -0.09375 to 0.09375
- linear_query_weight: bfloat16 [4096, 1024], P('sp', 'tp'), may hold values from -0.09375 to 0.09375
- linear_key_weight: bfloat16 [4096, 1024], P('sp', 'tp'), may hold values from -0.09375 to 0.09375
- linear_value_weight: bfloat16 [4096, 2048], P('sp', 'tp'), may hold values from -0.09375 to 0.09375
- decay_down_factor: bfloat16 [4096, 16], replicated, may hold values from -0.09375 to 0.09375
- decay_up_factor: bfloat16 [16, 1024], P(None, 'tp'), may hold values from -1.5 to 1.5
- decay_offset_bias: float32 [1024], P('tp'), may hold values from -0.5 to 9
- extra_fading_exponent: float32 [8192, 8], P(('fs', 'sp'), 'tp'), parts along dimension 0, may hold values from -1.5 to 0
- starting_state: float32 [8, 128, 256], P('tp'), may hold values from -12 to 12
- head_sink_logit: float32 [32], P('tp'), may hold values from 1 to 5
- linear_head_gain: float32 [256], replicated, may hold values from 0.1 to 1.9
- window_output_weight: bfloat16 [2048, 4096], P('tp', 'sp'), may hold values from -0.09375 to 0.09375
- linear_output_weight: bfloat16 [2048, 4096], P('tp', 'sp'), may hold values from -0.09375 to 0.09375
Outputs:
- mixer_output: bfloat16 [8192, 4096], P(('fs', 'sp', 'tp')), parts along dimension 0
The draws below stay inside these ranges and needn't reach their ends.
There are 4 independent parts, one for each index of `fs`. The reference program is written for one: setup_inputs(seed, part) draws one part's arguments, and reference() takes and returns one part's arrays. A program takes and returns all parts, laid end to end along the dimension named above; an argument that names none is the same for every part. Nothing has to cross between parts.
All inputs are finite; a program needn't handle non-finite values.
Results may differ from the reference program's by a relative error of at most 0.019.
Values may be sent and summed in bfloat16 or wider, within the bound.
A program may use at most 64 MiB of HBM per device.

```python
import jax
import jax.numpy as jnp
from jax import lax

D = 4096
QH = 32
KVH = 8
HD = 64
WINDOW = 128
GATED_MIXERS = 8
LOOKUP_FEATURES = 128
DV = 256
RANK = 16
SPAN = 64
T_DEV = 128
TOKENS = 2048
N_TP = 8


def draw_decay_offset_bias(key, part):
    key_flags, key_slow, key_quick = jax.random.split(key, 3)
    fast_share = 0.5
    is_quick = jax.random.uniform(key_flags, (GATED_MIXERS, 1)) < fast_share
    slow_values = jax.random.uniform(key_slow, (GATED_MIXERS, LOOKUP_FEATURES), minval=6.0, maxval=9.0)
    quick_values = jax.random.uniform(key_quick, (GATED_MIXERS, LOOKUP_FEATURES), minval=-0.5, maxval=1.0)
    return jnp.where(is_quick, quick_values, slow_values).reshape(GATED_MIXERS * LOOKUP_FEATURES).astype(jnp.float32)


def draw_extra_fading_exponent(key, part):
    key_rate, key_place, key_depth = jax.random.split(key, 3)
    block_count = TOKENS // T_DEV
    low_end = 0.25
    rates = jnp.exp(jax.random.uniform(key_rate, (block_count, GATED_MIXERS), minval=jnp.log(low_end), maxval=0.0))
    equilibrium_memory = jnp.repeat(-0.8 * rates / TOKENS, T_DEV, axis=0)
    element_indices = jax.random.randint(key_place, (2, GATED_MIXERS), 0, TOKENS)
    accrued_fading_totals = jnp.log(jax.random.uniform(key_depth, (2, GATED_MIXERS), minval=0.5, maxval=0.8))
    element_ordinals = jnp.arange(TOKENS, dtype=jnp.int32)[:, None, None]
    spike_contributions = jnp.sum(jnp.where(element_ordinals == element_indices[None], accrued_fading_totals[None], 0.0), axis=1)
    return (equilibrium_memory + spike_contributions).astype(jnp.float32)


def levels(rng, shape, shards, low, top_value):
    def one(axis_at, blocks):
        heights = jax.random.uniform(jax.random.fold_in(jax.random.fold_in(rng, 6), axis_at), (blocks,), jnp.float32, low / len(shards), top_value / len(shards))
        return jnp.repeat(jnp.exp(heights), shape[axis_at] // blocks).reshape((-1,) + (1,) * (len(shape) - axis_at - 1))

    factor_of = one(*shards[0])
    for cut in shards[1:]:
        factor_of = factor_of * one(*cut)
    return factor_of


def scatter_about(stream_key, dims, spread, bound, shards=(), kind=jnp.bfloat16):
    level = levels(stream_key, dims, shards, -0.22, 0.18) if shards else 1.0
    values = jax.random.normal(stream_key, dims, jnp.float32) * spread * level
    return jnp.minimum(jnp.maximum(values, -bound), bound).astype(kind)


def setup_inputs(seed: int = 0, part: int = 0) -> dict:
    seeds = jax.random.split(jax.random.key(seed), 18)
    part_splits = jax.random.split(jax.random.fold_in(seeds[17], part), 18)
    activations = scatter_about(part_splits[0], (TOKENS, D), 1.0, 6.0, ((0, 16), (1, 8)))
    input_norm_gain = jnp.clip(1.0 + 0.18 * jax.random.normal(seeds[1], (D,), jnp.float32), 0.1, 1.9)
    window_query_weight = scatter_about(seeds[2], (D, QH * HD), D ** -0.5, 0.09375, ((0, 16), (1, 8)))
    window_key_weight = scatter_about(seeds[3], (D, KVH * HD), D ** -0.5, 0.09375, ((0, 16), (1, 8)))
    window_value_weight = scatter_about(seeds[4], (D, KVH * HD), D ** -0.5, 0.09375, ((0, 16), (1, 8)))
    linear_query_weight = scatter_about(seeds[5], (D, GATED_MIXERS * LOOKUP_FEATURES), D ** -0.5, 0.09375, ((0, 16), (1, 8)))
    linear_key_weight = scatter_about(seeds[6], (D, GATED_MIXERS * LOOKUP_FEATURES), D ** -0.5, 0.09375, ((0, 16), (1, 8)))
    linear_value_weight = scatter_about(seeds[7], (D, GATED_MIXERS * DV), D ** -0.5, 0.09375, ((0, 16), (1, 8)))
    decay_down_factor = scatter_about(seeds[8], (D, RANK), D ** -0.5, 0.09375)
    decay_up_factor = scatter_about(seeds[9], (RANK, GATED_MIXERS * LOOKUP_FEATURES), RANK ** -0.5, 1.5, ((1, 8),))
    decay_offset_bias = draw_decay_offset_bias(jax.random.fold_in(seeds[17], 71), part)
    extra_fading_exponent = draw_extra_fading_exponent(jax.random.fold_in(jax.random.fold_in(seeds[17], part), 71), part)
    starting_state = scatter_about(seeds[12], (GATED_MIXERS, LOOKUP_FEATURES, DV), 2.0, 12.0, ((0, 8),), jnp.float32)
    head_sink_logit = jnp.clip(1.0 + 4.0 * jax.random.uniform(seeds[13], (QH,), jnp.float32) ** levels(seeds[13], (QH,), ((0, 8),), -0.2, 0.2), 1.0, 5.0)
    linear_head_gain = jnp.clip(1.0 + 0.18 * jax.random.normal(seeds[14], (DV,), jnp.float32), 0.1, 1.9)
    window_output_weight = scatter_about(seeds[15], (QH * HD, D), (QH * HD + GATED_MIXERS * DV) ** -0.5, 0.09375, ((0, 8), (1, 16)))
    linear_output_weight = scatter_about(seeds[16], (GATED_MIXERS * DV, D), (QH * HD + GATED_MIXERS * DV) ** -0.5, 0.09375, ((0, 8), (1, 16)))
    return {"activations": activations, "input_norm_gain": input_norm_gain, "window_query_weight": window_query_weight, "window_key_weight": window_key_weight, "window_value_weight": window_value_weight, "linear_query_weight": linear_query_weight, "linear_key_weight": linear_key_weight, "linear_value_weight": linear_value_weight, "decay_down_factor": decay_down_factor, "decay_up_factor": decay_up_factor, "decay_offset_bias": decay_offset_bias, "extra_fading_exponent": extra_fading_exponent, "starting_state": starting_state, "head_sink_logit": head_sink_logit, "linear_head_gain": linear_head_gain, "window_output_weight": window_output_weight, "linear_output_weight": linear_output_weight}


EPS = 1e-05
FADING_SOFTNESS = 16.0
HIGH_PRECISION = lax.Precision.HIGHEST

def window_reference(near_query, near_keys, near_values, head_sink_logit):
    stream_extent = near_query.shape[0]
    blocks = stream_extent // WINDOW
    groups = QH // KVH
    zeros_front = jnp.zeros((WINDOW, KVH * HD), jnp.float32)

    def banded(current):
        extended = jnp.concatenate([zeros_front, current.astype(jnp.float32)], axis=0)
        earlier = extended[:stream_extent].reshape(blocks, WINDOW, KVH, HD)
        present = extended[WINDOW:].reshape(blocks, WINDOW, KVH, HD)
        return jnp.concatenate([earlier, present], axis=1)
    key_band = banded(near_keys)
    value_band = banded(near_values)
    queries = near_query.astype(jnp.float32).reshape(blocks, WINDOW, KVH, groups, HD)
    scores = jnp.einsum('nqhgd,nkhd->hgnqk', queries, key_band, precision=HIGH_PRECISION) * HD ** (-0.5)
    head_ids = jnp.arange(QH, dtype=jnp.int32)
    slopes = jnp.exp2(-8.0 * (head_ids + 1).astype(jnp.float32) / QH).reshape(KVH, groups)
    query_pos = jnp.arange(WINDOW, dtype=jnp.int32)
    key_pos = jnp.arange(2 * WINDOW, dtype=jnp.int32)
    distance = query_pos[:, None] - key_pos[None, :] + WINDOW
    start_pos = (jnp.arange(blocks, dtype=jnp.int32) - 1) * WINDOW
    absolute = start_pos[:, None] + key_pos[None, :]
    allowed = ((distance >= 0) & (distance < WINDOW))[None] & (absolute >= 0)[:, None, :]
    biased = scores - slopes[:, :, None, None, None] * distance.astype(jnp.float32)
    weights = jnp.where(allowed, jnp.exp(biased), 0.0)
    denominator = lax.optimization_barrier(jnp.sum(weights, axis=-1, keepdims=True)) + jnp.exp(head_sink_logit.reshape(KVH, groups))[:, :, None, None, None]
    attention = (weights / denominator).astype(jnp.bfloat16)
    attended = jnp.einsum('hgnqk,nkhd->nqhgd', attention.astype(jnp.float32), value_band, precision=HIGH_PRECISION)
    return attended.reshape(stream_extent, QH * HD).astype(jnp.bfloat16)

def linear_reference(gated_query, gated_keys, gated_values, fading_exponent, linear_head_gain, starting_state):
    stream_extent = gated_query.shape[0]
    span_count = stream_extent // SPAN
    scaled_query = gated_query.astype(jnp.float32).reshape(span_count, SPAN, GATED_MIXERS, LOOKUP_FEATURES) * LOOKUP_FEATURES ** (-0.5)
    keys_wide = gated_keys.astype(jnp.float32).reshape(span_count, SPAN, GATED_MIXERS, LOOKUP_FEATURES)
    values_wide = gated_values.astype(jnp.float32).reshape(span_count, SPAN, GATED_MIXERS, DV)
    running = jnp.cumsum(fading_exponent.reshape(span_count, SPAN, GATED_MIXERS, LOOKUP_FEATURES), axis=1)
    span_end = running[:, -1]
    query_with_decay = scaled_query * jnp.exp(running)
    inverse_keys = keys_wide * jnp.exp(-running)
    ending_keys = keys_wide * jnp.exp(span_end[:, None] - running)
    inner = jnp.einsum('nchk,nshk->nhcs', query_with_decay, inverse_keys, precision=HIGH_PRECISION)
    lower = jnp.tril(jnp.ones((SPAN, SPAN), dtype=bool))
    inner = jnp.where(lower, inner, 0.0)
    within = jnp.einsum('nhcs,nshv->nchv', inner, values_wide, precision=HIGH_PRECISION)

    def advance(running_state, inputs):
        query_portion, key_portion, value_portion, scale_factor = inputs
        layer_output = jnp.einsum('fmy,mys->fms', query_portion, running_state, precision=HIGH_PRECISION)
        running_state = running_state * scale_factor[..., None] + jnp.einsum('gxp,gxz->xpz', key_portion, value_portion, precision=HIGH_PRECISION)
        return (running_state, layer_output)
    start_state = starting_state.astype(jnp.float32)
    final_state, carried = lax.scan(advance, start_state, (query_with_decay, ending_keys, values_wide, jnp.exp(span_end)))
    flat = (within + carried).reshape(stream_extent, GATED_MIXERS, DV)
    normal = flat * lax.rsqrt(lax.optimization_barrier(jnp.mean(flat * flat, axis=-1, keepdims=True)) + EPS) * linear_head_gain
    return normal.reshape(stream_extent, GATED_MIXERS * DV).astype(jnp.bfloat16)

def reference(activations, input_norm_gain, window_query_weight, window_key_weight, window_value_weight, linear_query_weight, linear_key_weight, linear_value_weight, decay_down_factor, decay_up_factor, decay_offset_bias, extra_fading_exponent, starting_state, head_sink_logit, linear_head_gain, window_output_weight, linear_output_weight):
    widened = activations.astype(jnp.float32)
    normed = (widened * lax.rsqrt(lax.optimization_barrier(jnp.mean(widened * widened, axis=1, keepdims=True)) + EPS) * input_norm_gain).astype(jnp.bfloat16)

    def project(matrix):
        return jnp.dot(normed, matrix, preferred_element_type=jnp.float32).astype(jnp.bfloat16)
    near_query = project(window_query_weight)
    near_keys = project(window_key_weight)
    near_values = project(window_value_weight)
    gated_query = project(linear_query_weight)
    gated_keys = project(linear_key_weight)
    gated_values = project(linear_value_weight)
    low_rank = project(decay_down_factor)
    attention_energies = jnp.dot(low_rank, decay_up_factor, preferred_element_type=jnp.float32) + decay_offset_bias
    stream_extent = normed.shape[0]
    fading_exponent = (jax.nn.log_sigmoid(attention_energies) / FADING_SOFTNESS).reshape(stream_extent, GATED_MIXERS, LOOKUP_FEATURES) + extra_fading_exponent[:, :, None]
    near_out = window_reference(near_query, near_keys, near_values, head_sink_logit)
    gated_out = linear_reference(gated_query, gated_keys, gated_values, fading_exponent, linear_head_gain, starting_state)
    window_cols = QH * HD // N_TP
    linear_cols = GATED_MIXERS * DV // N_TP
    accumulated = jnp.zeros((stream_extent, D), jnp.float32)
    for member in range(N_TP):
        first_w = member * window_cols
        first_l = member * linear_cols
        partial_value = jnp.dot(near_out[:, first_w:first_w + window_cols], window_output_weight[first_w:first_w + window_cols], preferred_element_type=jnp.float32)
        partial_value = partial_value + jnp.dot(gated_out[:, first_l:first_l + linear_cols], linear_output_weight[first_l:first_l + linear_cols], preferred_element_type=jnp.float32)
        rounded = lax.optimization_barrier(partial_value.astype(jnp.bfloat16))
        accumulated = accumulated + rounded.astype(jnp.float32)
    return accumulated.astype(jnp.bfloat16)
```

```python
import functools

import jax
import jax.numpy as jnp
from jax import lax
from jax.experimental import pallas as pl
from jax.experimental.pallas import tpu as pltpu
from jax.sharding import PartitionSpec as P

MESH = pl.DeviceIdType.MESH
HD = 64
HEADS = 4
LK = 128
DV = 256
SPAN = 64
TOK = 128
FEAT = 512
ROWS = 256
RANK = 16
EPS = 1e-05
HIGH = lax.Precision.HIGHEST
F32 = jnp.float32
BF16 = jnp.bfloat16
C_LK, C_LV, C_LQ, C_WQ, C_KV, C_END = 0, 128, 384, 512, 768, 896
STREAMS = ((0, 384), (384, 512))


def over(a, b, ca, cb, precision=None):
    return lax.dot_general(
        a, b, (((ca,), (cb,)), ((), ())), preferred_element_type=F32, precision=precision
    )


def kernel(
    SP, FS, TP,
    x_ref, gain_ref, wq_ref, wkt_ref, wvt_ref, lq_ref, lk_ref, lv_ref, ddt_ref, up_ref,
    bias_ref, extra_ref, start_ref, sink_ref, lgain_ref, wow_ref, wol_ref,
    out_ref,
    xs, xg, aux, wg, wo, wcat, rs_send, rs_recv, kv, st_send, st_recv, dlog, pre_send,
    pre_recv, startt, og, po, xr_recv, fin_send, fin_recv,
    ring_s, ring_r, y_s, y_r, x_s, x_r, a_s, a_r, d_s, d_r, rs_s, rs_r, kv_s, kv_r,
    st_s, st_r, pre_s, pre_r, og_s, og_r, xr_s, xr_r, fin_s, fin_r,
):
    s, f, t = lax.axis_index("sp"), lax.axis_index("fs"), lax.axis_index("tp")
    q = ROWS // FS
    ft = FEAT // FS
    vr = DV // SP
    tr = TOK // TP
    dim = FEAT * TP
    right, left = lax.rem(s + 1, SP), lax.rem(s + SP - 1, SP)
    pending = []

    def peer(me, offset, count):
        return lax.rem(me + offset, count)

    def copy(src, dst, send_sem, recv_sem, **device):
        return pltpu.make_async_remote_copy(
            src_ref=src, dst_ref=dst, send_sem=send_sem, recv_sem=recv_sem,
            device_id=device, device_id_type=MESH,
        )

    def send(src, dst, send_sem, recv_sem, **device):
        c = copy(src, dst, send_sem, recv_sem, **device)
        c.start()
        pending.append(c)

    def arrived(dst, send_sem, recv_sem, **device):
        copy(dst, dst, send_sem, recv_sem, **device).wait_recv()

    barrier = pltpu.get_barrier_semaphore()
    pl.semaphore_signal(barrier, inc=1, device_id={"sp": right}, device_id_type=MESH)
    pl.semaphore_signal(barrier, inc=1, device_id={"sp": left}, device_id_type=MESH)
    for o in range(1, FS):
        pl.semaphore_signal(barrier, inc=1, device_id={"fs": peer(f, o, FS)}, device_id_type=MESH)
    for o in range(1, TP):
        pl.semaphore_signal(barrier, inc=1, device_id={"tp": peer(t, o, TP)}, device_id_type=MESH)

    mine = pl.ds(pl.multiple_of(s * q, q), q)
    part = pl.ds(pl.multiple_of(f * q, q), q)
    wg[mine, C_LK:C_LV] = lk_ref[part, :]
    wg[mine, C_LV:C_LQ] = lv_ref[part, :]
    wg[mine, C_LQ:C_WQ] = lq_ref[part, :]
    wg[mine, C_WQ:C_KV] = wq_ref[part, :]
    both = jnp.concatenate([wkt_ref[...], wvt_ref[...]], axis=0).astype(F32).T.astype(BF16)
    for k in range(FS):
        @pl.when(f == k)
        def _():
            wg[mine, C_KV:C_END] = both[k * q:(k + 1) * q, :]
            wo[s] = jnp.concatenate(
                [wow_ref[:, k * q:(k + 1) * q], wol_ref[:, k * q:(k + 1) * q]], axis=1
            )

    pl.semaphore_wait(barrier, 2 + (FS - 1) + (TP - 1))

    half = SP // 2

    def chunk(stream, z):
        if stream == 2:
            return wo.at[z]
        at, width = STREAMS[stream]
        return wg.at[pl.ds(pl.multiple_of(z * q, q), q), pl.ds(at, width)]

    def ring_step(stream, k):
        for d in range(2):
            to, back = (right, left) if d == 0 else (left, right)
            count = half if d == 0 else SP - 1 - half
            z = lax.rem(s + SP - k, SP) if d == 0 else lax.rem(s + k, SP)
            if 1 <= k <= count:
                arrived(chunk(stream, z), ring_s.at[stream, d, k - 1],
                        ring_r.at[stream, d, k - 1], sp=back)
            if k < count:
                send(chunk(stream, z), chunk(stream, z), ring_s.at[stream, d, k],
                     ring_r.at[stream, d, k], sp=to)

    done = [0]

    def third():
        if done[0] <= half:
            ring_step(2, done[0])
            done[0] += 1

    ring_step(0, 0)
    ring_step(1, 0)

    xf = x_ref[...].astype(F32)
    rows = FEAT // 128
    gain = jnp.concatenate(
        [gain_ref[pl.ds(t * rows + k, 1), :] for k in range(rows)], axis=1
    )
    xw = (xf * gain).astype(BF16)
    here = pl.ds(pl.multiple_of(t * ft, ft), ft)
    for k in range(FS):
        cut = jnp.concatenate(
            [xw[:, k * q:(k + 1) * q], xw[:, ROWS + k * q:ROWS + (k + 1) * q]], axis=1
        )
        xs[k] = cut

        @pl.when(f == k)
        def _():
            xg[k, :, here] = cut
    for o in range(1, FS):
        to = peer(f, o, FS)
        send(xs.at[to], xg.at[f, :, here], y_s.at[o - 1], y_r.at[o - 1], fs=to)
    dd = ddt_ref[:, pl.ds(pl.multiple_of(t * FEAT, FEAT), FEAT)]
    aux[t, :RANK, :] = over(dd, xw, 1, 1)
    aux[t, RANK:, :] = over(jnp.ones((8, FEAT), F32), xf * xf, 1, 1, HIGH)
    for o in range(1, TP):
        send(aux.at[t], aux.at[t], a_s.at[o - 1], a_r.at[o - 1], tp=peer(t, o, TP))

    ring_step(0, 1)
    ring_step(1, 1)
    for o in range(1, FS):
        came = peer(f, FS - o, FS)
        arrived(xg.at[came, :, here], y_s.at[o - 1], y_r.at[o - 1], fs=came)
    for o in range(1, TP):
        send(xg.at[:, :, here], xg.at[:, :, here], x_s.at[o - 1], x_r.at[o - 1],
             tp=peer(t, o, TP))
    startt[...] = start_ref[...].T

    for k in range(2, half + 1):
        ring_step(0, k)
        ring_step(1, k)
        if k >= half // 2:
            third()

    for o in range(1, TP):
        came = peer(t, TP - o, TP)
        arrived(aux.at[came], a_s.at[o - 1], a_r.at[o - 1], tp=came)
    sums = aux[0]
    for k in range(1, TP):
        sums = sums + aux[k]
    scale_rows = lax.rsqrt(sums[RANK:, :] / dim + EPS)
    eighth = jnp.full((8, 128), 0.125, F32)
    scale = over(scale_rows, eighth, 0, 0, HIGH)
    low = (sums[:RANK, :] * scale_rows[0:1, :]).astype(BF16)
    energies = over(low, up_ref[...], 0, 0) + bias_ref[...]
    extra = over(jnp.broadcast_to(extra_ref[...], (8, 128)), eighth, 0, 0, HIGH)
    fading = (
        jnp.minimum(energies, 0.0) - jnp.log1p(jnp.exp(-jnp.abs(energies)))
    ) / 16.0 + extra
    ri = lax.broadcasted_iota(jnp.int32, (TOK, TOK), 0)
    ci = lax.broadcasted_iota(jnp.int32, (TOK, TOK), 1)
    tri = ((ri >= ci) & ((ri < SPAN) | (ci >= SPAN))).astype(F32)
    running = over(tri, fading, 1, 0, HIGH)
    end0, end1 = running[SPAN - 1:SPAN, :], running[TOK - 1:TOK, :]
    dlog[s] = jnp.broadcast_to(end0 + end1, (8, 128))
    for o in range(1, SP):
        send(dlog.at[s], dlog.at[s], d_s.at[o - 1], d_r.at[o - 1], sp=peer(s, o, SP))
    for o in range(1, TP):
        came = peer(t, TP - o, TP)
        there = pl.ds(pl.multiple_of(came * ft, ft), ft)
        arrived(xg.at[:, :, there], x_s.at[o - 1], x_r.at[o - 1], tp=came)

    owns = []
    for stream, (at, width) in enumerate(STREAMS):
        cols = pl.ds(at, width)
        for o in list(range(1, FS)) + [0]:
            to = peer(f, o, FS)
            product = over(xg[to], wg[:, at:at + width], 1, 0)
            if o == 0:
                owns.append(product)
            else:
                rs_send[o - 1, :, at:at + width] = product.astype(BF16)
                send(rs_send.at[o - 1, :, cols], rs_recv.at[o - 1, :, cols],
                     rs_s.at[stream, o - 1], rs_r.at[stream, o - 1], fs=to)

    def reduced(stream):
        at, width = STREAMS[stream]
        total = owns[stream]
        for o in range(1, FS):
            came = peer(f, FS - o, FS)
            arrived(rs_recv.at[o - 1, :, pl.ds(at, width)], rs_s.at[stream, o - 1],
                    rs_r.at[stream, o - 1], fs=came)
            total = total + rs_recv[o - 1, :, at:at + width].astype(F32)
        wide = jnp.concatenate([scale] * (width // 128), axis=1)
        return (total * wide).astype(BF16)

    third()
    first = reduced(0)
    keys = first[:, C_LK:C_LV].astype(F32)
    values = first[:, C_LV:C_LQ].astype(F32)
    grow = jnp.exp(running)
    ends = jnp.where(ri < SPAN, end0, end1)
    ending = keys * jnp.exp(ends - running)
    state0 = over(values[:SPAN], ending[:SPAN], 0, 0, HIGH)
    state1 = state0 * jnp.exp(end1) + over(values[SPAN:], ending[SPAN:], 0, 0, HIGH)
    packed = state1.astype(BF16)
    st_send[...] = packed.reshape(SP, vr, LK)
    st_recv[s] = st_send[s]
    for o in range(1, SP):
        to = peer(s, o, SP)
        send(st_send.at[to], st_recv.at[s], st_s.at[o - 1], st_r.at[o - 1], sp=to)

    third()
    second = reduced(1)
    kv[1] = second[:, C_KV - C_LQ:]
    send(kv.at[1], kv.at[0], kv_s, kv_r, sp=right)
    inverse = keys * jnp.exp(-running)
    query = second[:, :C_WQ - C_LQ].astype(F32) * (LK ** -0.5) * grow
    raws = []
    for n in range(2):
        span = slice(n * SPAN, (n + 1) * SPAN)
        inner = over(query[span], inverse[span], 1, 1, HIGH)
        inner = jnp.where(ri[:SPAN, :SPAN] >= ci[:SPAN, :SPAN], inner, 0.0)
        raws.append(over(inner, values[span], 1, 0, HIGH))
    raws[1] = raws[1] + over(query[SPAN:], state0, 1, 1, HIGH)

    for o in range(1, SP):
        came = peer(s, SP - o, SP)
        arrived(dlog.at[came], d_s.at[o - 1], d_r.at[o - 1], sp=came)
    for o in range(1, SP):
        came = peer(s, SP - o, SP)
        arrived(st_recv.at[came], st_s.at[o - 1], st_r.at[o - 1], sp=came)
    state = startt[pl.ds(pl.multiple_of(s * vr, vr), vr), :]
    for k in range(SP):
        pre_send[k] = state.astype(BF16)
        if k < SP - 1:
            state = state * jnp.exp(dlog[k][0:1, :]) + st_recv[k].astype(F32)
    pre_recv[s] = pre_send[s]
    for o in range(1, SP):
        to = peer(s, o, SP)
        send(pre_send.at[to], pre_recv.at[s], pre_s.at[o - 1], pre_r.at[o - 1], sp=to)

    third()
    arrived(kv.at[0], kv_s, kv_r, sp=left)
    kvs = jnp.concatenate([kv[0], kv[1]], axis=0)
    kw, vw = kvs[:, :HD], kvs[:, HD:]
    qi = lax.broadcasted_iota(jnp.int32, (TOK, 2 * TOK), 0)
    ki = lax.broadcasted_iota(jnp.int32, (TOK, 2 * TOK), 1)
    distance = qi - ki + TOK
    allowed = (distance >= 0) & (distance < TOK) & ((ki >= TOK) | (s > 0))
    far = distance.astype(F32)
    nears = []
    for h in range(HEADS):
        qh = second[:, C_WQ - C_LQ + h * HD:C_WQ - C_LQ + (h + 1) * HD]
        scores = over(qh, kw, 1, 1) * (HD ** -0.5)
        head = jnp.full((1, 1), t * HEADS + h + 1, jnp.int32).astype(F32)
        slope = jnp.exp2(-8.0 * head / (HEADS * TP))
        weights = jnp.where(allowed, jnp.exp(scores - slope * far), 0.0)
        total = jnp.sum(weights, axis=1, keepdims=True) + jnp.exp(sink_ref[0:1, h:h + 1])
        probs = (weights / total).astype(BF16)
        nears.append(over(probs, vw, 1, 0).astype(BF16))
    og[f, :, :HEADS * HD] = jnp.concatenate(nears, axis=1)

    def share(part_index):
        lanes = pl.ds(part_index * DV, DV)
        for o in range(1, FS):
            send(og.at[f, :, lanes], og.at[f, :, lanes], og_s.at[part_index, o - 1],
                 og_r.at[part_index, o - 1], fs=peer(f, o, FS))

    def shared(part_index):
        lanes = pl.ds(part_index * DV, DV)
        for o in range(1, FS):
            came = peer(f, FS - o, FS)
            arrived(og.at[came, :, lanes], og_s.at[part_index, o - 1],
                    og_r.at[part_index, o - 1], fs=came)

    share(0)
    while done[0] <= half:
        third()
    per = 128 // q
    for k in range(SP // per):
        for side in range(2):
            wcat[side * DV:(side + 1) * DV, k * 128:(k + 1) * 128] = jnp.concatenate(
                [wo[k * per + i][:, side * q:(side + 1) * q] for i in range(per)], axis=1
            )

    for o in range(1, SP):
        came = peer(s, SP - o, SP)
        arrived(pre_recv.at[came], pre_s.at[o - 1], pre_r.at[o - 1], sp=came)
    before = pre_recv[...].reshape(DV, LK).astype(F32)
    raws[0] = raws[0] + over(query[:SPAN], before, 1, 1, HIGH)
    raws[1] = raws[1] + over(query[SPAN:] * jnp.exp(end0), before, 1, 1, HIGH)
    raw = jnp.concatenate(raws, axis=0)
    gated = raw * lax.rsqrt(jnp.mean(raw * raw, axis=1, keepdims=True) + EPS) * lgain_ref[...]
    og[f, :, DV:] = gated.astype(BF16)
    share(1)
    shared(0)
    shared(1)

    heads = og[...].reshape(FS * TOK, 2 * DV)
    po[...] = over(heads, wcat[...], 1, 0).astype(BF16).reshape(FS, TOK, SP * q)
    for o in range(1, TP):
        to = peer(t, o, TP)
        send(po.at[:, pl.ds(pl.multiple_of(to * tr, tr), tr), :], xr_recv.at[o - 1],
             xr_s.at[o - 1], xr_r.at[o - 1], tp=to)
    total = po[:, pl.ds(pl.multiple_of(t * tr, tr), tr), :].astype(F32)
    for o in range(1, TP):
        came = peer(t, TP - o, TP)
        arrived(xr_recv.at[o - 1], xr_s.at[o - 1], xr_r.at[o - 1], tp=came)
        total = total + xr_recv[o - 1].astype(F32)
    fin_send[...] = total.astype(BF16)
    fin_recv[f] = fin_send[f]
    for o in range(1, FS):
        to = peer(f, o, FS)
        send(fin_send.at[to], fin_recv.at[f], fin_s.at[o - 1], fin_r.at[o - 1], fs=to)
    for o in range(1, FS):
        came = peer(f, FS - o, FS)
        arrived(fin_recv.at[came], fin_s.at[o - 1], fin_r.at[o - 1], fs=came)
    for z in range(SP):
        out_ref[:, z * ROWS:(z + 1) * ROWS] = jnp.concatenate(
            [fin_recv[k][:, z * q:(z + 1) * q] for k in range(FS)], axis=1
        )
    for c in pending:
        c.wait_send()


def local(SP, FS, TP, *arrays):
    (activations, input_norm_gain, wq, wk, wv, lq, lk, lv, down, up, bias, extra, start, sink,
     lgain, wow, wol) = arrays
    q, ft, vr, tr = ROWS // FS, FEAT // FS, DV // SP, TOK // TP
    half = SP // 2
    dma = pltpu.SemaphoreType.DMA
    operands = (
        activations, input_norm_gain.reshape(-1, 128), wq, wk.T, wv.T, lq, lk, lv, down.T, up,
        bias.reshape(1, -1), extra.reshape(1, -1), start.reshape(LK, DV), sink.reshape(1, -1),
        lgain.reshape(1, -1), wow, wol,
    )
    vmem = pl.BlockSpec(memory_space=pltpu.VMEM)
    return pl.pallas_call(
        functools.partial(kernel, SP, FS, TP),
        out_shape=jax.ShapeDtypeStruct((tr, SP * ROWS), BF16),
        in_specs=[vmem] * len(operands),
        out_specs=vmem,
        scratch_shapes=[
            pltpu.VMEM((FS, TOK, ft), BF16),
            pltpu.VMEM((FS, TOK, TP * ft), BF16),
            pltpu.VMEM((TP, RANK + 8, TOK), F32),
            pltpu.VMEM((SP * q, C_END), BF16),
            pltpu.VMEM((SP, 256, 2 * q), BF16),
            pltpu.VMEM((2 * DV, SP * q), BF16),
            pltpu.VMEM((FS - 1, TOK, C_END), BF16),
            pltpu.VMEM((FS - 1, TOK, C_END), BF16),
            pltpu.VMEM((2, TOK, 2 * HD), BF16),
            pltpu.VMEM((SP, vr, LK), BF16),
            pltpu.VMEM((SP, vr, LK), BF16),
            pltpu.VMEM((SP, 8, LK), F32),
            pltpu.VMEM((SP, vr, LK), BF16),
            pltpu.VMEM((SP, vr, LK), BF16),
            pltpu.VMEM((DV, LK), F32),
            pltpu.VMEM((FS, TOK, 2 * DV), BF16),
            pltpu.VMEM((FS, TOK, SP * q), BF16),
            pltpu.VMEM((TP - 1, FS, tr, SP * q), BF16),
            pltpu.VMEM((FS, tr, SP * q), BF16),
            pltpu.VMEM((FS, tr, SP * q), BF16),
            dma((3, 2, half)), dma((3, 2, half)),
            dma((FS - 1,)), dma((FS - 1,)),
            dma((TP - 1,)), dma((TP - 1,)),
            dma((TP - 1,)), dma((TP - 1,)),
            dma((SP - 1,)), dma((SP - 1,)),
            dma((2, FS - 1)), dma((2, FS - 1)),
            dma, dma,
            dma((SP - 1,)), dma((SP - 1,)),
            dma((SP - 1,)), dma((SP - 1,)),
            dma((2, FS - 1)), dma((2, FS - 1)),
            dma((TP - 1,)), dma((TP - 1,)),
            dma((FS - 1,)), dma((FS - 1,)),
        ],
        compiler_params=pltpu.CompilerParams(
            collective_id=0, has_side_effects=True, vmem_limit_bytes=60 * 1024 * 1024
        ),
    )(*operands)


def solution(mesh):
    placed = (
        P(("fs", "sp"), "tp"), P(), P("sp", "tp"), P("sp", "tp"), P("sp", "tp"), P("sp", "tp"),
        P("sp", "tp"), P("sp", "tp"), P(), P(None, "tp"), P("tp"), P(("fs", "sp"), "tp"),
        P("tp", None, None), P("tp"), P(), P("tp", "sp"), P("tp", "sp"),
    )
    sizes = (mesh.shape["sp"], mesh.shape["fs"], mesh.shape["tp"])
    return jax.shard_map(
        functools.partial(local, *sizes), mesh=mesh, in_specs=placed,
        out_specs=P(("fs", "sp", "tp"), None), check_vma=False,
    )
```

```python
import functools

import jax
import jax.numpy as jnp
from jax import lax
from jax.experimental import pallas as pl
from jax.experimental.pallas import tpu as pltpu
from jax.sharding import PartitionSpec as P

MESH = pl.DeviceIdType.MESH
HD = 64
HEADS = 4
LK = 128
DV = 256
SPAN = 64
TOK = 128
FEAT = 512
ROWS = 256
RANK = 16
EPS = 1e-05
HIGH = lax.Precision.HIGHEST
F32 = jnp.float32
BF16 = jnp.bfloat16
C_LK, C_LV, C_LQ, C_WQ, C_KV, C_END = 0, 128, 384, 512, 768, 896
RINGS = ((0, 384), (384, 512))
PARTS = ((0, 384), (768, 128), (384, 384))


def over(a, b, ca, cb, precision=None):
    return lax.dot_general(
        a, b, (((ca,), (cb,)), ((), ())), preferred_element_type=F32, precision=precision
    )


def kernel(
    SP, FS, TP,
    x_hbm, gain_hbm, wq_hbm, wkt_hbm, wvt_hbm, lq_hbm, lk_hbm, lv_hbm, ddt_hbm, up_hbm,
    bias_hbm, extra_hbm, start_hbm, sink_hbm, lgain_hbm, wow_hbm, wol_hbm,
    out_hbm,
    out_ref, x_ref, gain_ref, wkt_ref, wvt_ref, ddt_ref, up_ref, bias_ref, extra_ref, start_ref,
    sink_ref, lgain_ref, wow_ref, wol_ref,
    xs, xg, aux, wg, wo, wcat, rs_send, rs_recv, kv, st_send, st_recv, dlog, pre_send,
    pre_recv, startt, og, po, pr_recv, pr_send, xr_recv, fin,
    in_s, out_s, h_s, h_r, w_s, w_r, ring_s, ring_r, y_s, y_r, x_s, x_r, xf_s, xf_r, a_s, a_r, d_s, d_r, rs_s, rs_r, kv_s, kv_r,
    st_s, st_r, pre_s, pre_r, og_s, og_r, pr_s, pr_r, xr_s, xr_r, none_s, none_r,
):
    s, f, t = lax.axis_index("sp"), lax.axis_index("fs"), lax.axis_index("tp")
    q = ROWS // FS
    ft = FEAT // FS
    vr = DV // SP
    tr = TOK // TP
    dim = FEAT * TP
    X = TP // 2
    xi, core = t // 2, lax.rem(t, 2)
    twin = xi * 2 + 1 - core
    right, left = lax.rem(s + 1, SP), lax.rem(s + SP - 1, SP)

    def peer(me, offset, count):
        return lax.rem(me + offset, count)

    def copy(src, dst, send_sem, recv_sem, **device):
        return pltpu.make_async_remote_copy(
            src_ref=src, dst_ref=dst, send_sem=send_sem, recv_sem=recv_sem,
            device_id=device, device_id_type=MESH,
        )

    def send(src, dst, send_sem, recv_sem, **device):
        copy(src, dst, send_sem, recv_sem, **device).start()

    def arrived(ref, recv_sem):
        copy(ref, ref, none_s, recv_sem, tp=twin).wait_recv()

    def left_here(ref, send_sem):
        copy(ref, ref, send_sem, none_r, tp=twin).wait_send()

    barrier = pltpu.get_barrier_semaphore()
    pl.semaphore_signal(barrier, inc=1, device_id={"sp": right}, device_id_type=MESH)
    pl.semaphore_signal(barrier, inc=1, device_id={"sp": left}, device_id_type=MESH)
    for o in range(1, FS):
        pl.semaphore_signal(barrier, inc=1, device_id={"fs": peer(f, o, FS)}, device_id_type=MESH)
    for o in range(1, TP):
        pl.semaphore_signal(barrier, inc=1, device_id={"tp": peer(t, o, TP)}, device_id_type=MESH)

    mine = pl.ds(pl.multiple_of(s * q, q), q)
    part = pl.ds(pl.multiple_of(f * q, q), q)
    loads = []
    for src, dst in (
        (lk_hbm.at[part, :], wg.at[core, mine, pl.ds(C_LK, LK)]),
        (lv_hbm.at[part, :], wg.at[core, mine, pl.ds(C_LV, DV)]),
        (lq_hbm.at[part, :], wg.at[core, mine, pl.ds(C_LQ, LK)]),
        (wq_hbm.at[part, :], wg.at[core, mine, pl.ds(C_WQ, HEADS * HD)]),
        (wkt_hbm, wkt_ref), (wvt_hbm, wvt_ref), (x_hbm, x_ref), (gain_hbm, gain_ref),
        (ddt_hbm, ddt_ref), (wow_hbm, wow_ref), (wol_hbm, wol_ref), (start_hbm, start_ref),
        (up_hbm, up_ref), (bias_hbm, bias_ref), (extra_hbm, extra_ref), (sink_hbm, sink_ref),
        (lgain_hbm, lgain_ref),
    ):
        c = pltpu.make_async_copy(src, dst, in_s.at[len(loads)])
        c.start()
        loads.append(c)
    for c in loads[:6]:
        c.wait()
    both = jnp.concatenate([wkt_ref[...], wvt_ref[...]], axis=0).astype(F32).T.astype(BF16)
    for k in range(FS):
        @pl.when(f == k)
        def _():
            wg[core, mine, C_KV:C_END] = both[k * q:(k + 1) * q, :]

    pl.semaphore_wait(barrier, 2 + (FS - 1) + (TP - 1))

    half = SP // 2

    both_cores = pl.ds(0, 2)

    def chunk(stream, z, cores):
        if stream >= 4:
            return wo.at[cores, z, pl.ds(stream % 2 * LK, LK)]
        at, width = RINGS[stream // 2]
        h = q // 2
        rows = pl.ds(pl.multiple_of(z * q + stream % 2 * h, h), h)
        return wg.at[cores, rows, pl.ds(at, width)]

    groups = (0, 0, 1, 1, 2, 3)

    def carrier(group):
        return (1, 0, 1, 0)[group]

    def carries(group):
        return core == carrier(group)

    def own_copy(group):
        guest = 1 - carrier(group)
        if group >= 2:
            src = wo.at[guest, s, pl.ds((group - 2) * LK, LK)]
        else:
            at, width = RINGS[group]
            src = wg.at[guest, mine, pl.ds(at, width)]
        return copy(src, src, h_s.at[group], h_r.at[group], tp=twin)

    counts = (half, SP - 1 - half)

    def ring_copy(stream, d, k):
        z = lax.rem(s + SP - k, SP) if d == 0 else lax.rem(s + k, SP)
        ref = chunk(stream, z, both_cores)
        return copy(ref, ref, ring_s.at[groups[stream]], ring_r.at[stream, d, k],
                    sp=right if d == 0 else left)

    def from_ring(stream, d, k):
        arrived(chunk(stream, 0, both_cores), ring_r.at[stream, d, k])

    def twin_copy(stream, d, k):
        z = lax.rem(s + SP - 1 - k, SP) if d == 0 else lax.rem(s + k + 1, SP)
        ref = chunk(stream, z, 1 - carrier(groups[stream]))
        return copy(ref, ref, w_s.at[groups[stream]], w_r.at[groups[stream]], tp=twin)

    def ring_step(stream, k):
        @pl.when(carries(groups[stream]))
        def _():
            if k == 0 and (stream % 2 == 0 or stream > 3):
                own_copy(groups[stream]).wait_recv()
            for d in range(2):
                if 1 <= k <= counts[d]:
                    from_ring(stream, d, k - 1)
                if k < counts[d]:
                    ring_copy(stream, d, k).start()
                if 1 <= k <= counts[d]:
                    twin_copy(stream, d, k - 1).start()

    def many(group, cores):
        if group >= 2:
            return wo.at[cores, pl.ds(0, SP - 1), pl.ds((group - 2) * LK, LK)]
        at, width = RINGS[group]
        return wg.at[cores, pl.ds(0, (SP - 1) * q), pl.ds(at, width)]

    def landed(group):
        @pl.when(jnp.logical_not(carries(group)))
        def _():
            arrived(many(group, 1 - carrier(group)), w_r.at[group])

    done = [0]

    def lagging():
        if done[0] <= half:
            ring_step(4, done[0])
            ring_step(5, done[0])
            done[0] += 1

    def second_group(k):
        ring_step(2, k)
        ring_step(3, k)

    def tick(k):
        ring_step(0, k)
        ring_step(1, k)
        if k < half - 1:
            second_group(k)
        if k >= 2 and k % 2 == 0:
            lagging()

    @pl.when(core == 0)
    def _():
        own_copy(0).start()

    @pl.when(core == 1)
    def _():
        own_copy(1).start()

    tick(0)

    for c in loads[6:11]:
        c.wait()
    for k in range(FS):
        @pl.when(f == k)
        def _():
            wo[core, s] = jnp.concatenate(
                [wow_ref[:, k * q:(k + 1) * q], wol_ref[:, k * q:(k + 1) * q]], axis=1
            )
    xf = x_ref[...].astype(F32)
    @pl.when(core == 0)
    def _():
        own_copy(2).start()

    @pl.when(core == 1)
    def _():
        own_copy(3).start()

    rows = FEAT // 128
    gain = jnp.concatenate(
        [gain_ref[pl.ds(t * rows + k, 1), :] for k in range(rows)], axis=1
    )
    xw = (xf * gain).astype(BF16)
    here = pl.ds(pl.multiple_of(t * ft, ft), ft)
    for k in range(FS):
        cut = jnp.concatenate(
            [xw[:, k * q:(k + 1) * q], xw[:, ROWS + k * q:ROWS + (k + 1) * q]], axis=1
        )
        xs[k] = cut

        @pl.when(f == k)
        def _():
            xg[k, :, here] = cut
    for o in range(1, FS):
        to = peer(f, o, FS)
        send(xs.at[to], xg.at[f, :, here], y_s, y_r, fs=to)
    dd = ddt_ref[:, pl.ds(pl.multiple_of(t * FEAT, FEAT), FEAT)]
    aux[t, :RANK, :] = over(dd, xw, 1, 1)
    aux[t, RANK:, :] = over(jnp.ones((8, FEAT), F32), xf * xf, 1, 1, HIGH)
    for o in range(1, TP):
        send(aux.at[t], aux.at[t], a_s, a_r, tp=peer(t, o, TP))

    tick(1)
    arrived(xg.at[pl.ds(0, FS - 1), :, here], y_r)
    for o in range(1, X):
        send(xg.at[:, :, here], xg.at[:, :, here], x_s, x_r.at[o - 1],
             tp=peer(xi, o, X) * 2 + core)
    send(xg.at[:, :, here], xg.at[:, :, here], x_s, x_r.at[X - 1], tp=twin)
    for c in loads[11:]:
        c.wait()
    startt[...] = start_ref[...].T
    early = max(2, 3 * half // 4)
    for k in range(2, early):
        tick(k)

    def lanes_of(device):
        return pl.ds(pl.multiple_of(device * ft, ft), ft)

    for o in range(1, X):
        came = peer(xi, X - o, X) * 2 + core
        chunk_x = xg.at[:, :, lanes_of(came)]
        arrived(chunk_x, x_r.at[o - 1])
        send(chunk_x, chunk_x, xf_s, xf_r, tp=twin)
    tick(early)
    arrived(aux.at[pl.ds(0, TP - 1)], a_r)
    sums = aux[0]
    for k in range(1, TP):
        sums = sums + aux[k]
    scale_rows = lax.rsqrt(sums[RANK:, :] / dim + EPS)
    eighth = jnp.full((8, 128), 0.125, F32)
    scale = over(scale_rows, eighth, 0, 0, HIGH)
    low = (sums[:RANK, :] * scale_rows[0:1, :]).astype(BF16)
    energies = over(low, up_ref[...], 0, 0) + bias_ref[...]
    extra = over(jnp.broadcast_to(extra_ref[...], (8, 128)), eighth, 0, 0, HIGH)
    fading = (
        jnp.minimum(energies, 0.0) - jnp.log1p(jnp.exp(-jnp.abs(energies)))
    ) / 16.0 + extra
    ri = lax.broadcasted_iota(jnp.int32, (TOK, TOK), 0)
    ci = lax.broadcasted_iota(jnp.int32, (TOK, TOK), 1)
    tri = ((ri >= ci) & ((ri < SPAN) | (ci >= SPAN))).astype(F32)
    running = over(tri, fading, 1, 0, HIGH)
    end0, end1 = running[SPAN - 1:SPAN, :], running[TOK - 1:TOK, :]
    dlog[s] = jnp.broadcast_to(end0 + end1, (8, 128))
    for k in range(early + 1, half + 1):
        tick(k)
    landed(0)
    arrived(xg.at[:, :, lanes_of(twin)], x_r.at[X - 1])
    if X > 1:
        arrived(xg.at[:, :, pl.ds(0, (X - 1) * ft)], xf_r)

    owns = []

    def project(part_index):
        at, width = PARTS[part_index]
        cols = pl.ds(at, width)
        for o in list(range(1, FS)) + [0]:
            to = peer(f, o, FS)
            product = over(xg[to], wg[core, :, at:at + width], 1, 0)
            if o == 0:
                owns.append(product)
            else:
                rs_send[o - 1, :, at:at + width] = product.astype(BF16)
                send(rs_send.at[o - 1, :, cols], rs_recv.at[o - 1, :, cols],
                     rs_s, rs_r.at[part_index], fs=to)

    def reduced(part_index):
        at, width = PARTS[part_index]
        total = owns[part_index]
        arrived(rs_recv.at[:, :, pl.ds(at, width)], rs_r.at[part_index])
        for o in range(1, FS):
            total = total + rs_recv[o - 1, :, at:at + width].astype(F32)
        wide = jnp.concatenate([scale] * (width // 128), axis=1)
        return (total * wide).astype(BF16)

    project(0)
    for o in range(1, SP):
        send(dlog.at[s], dlog.at[s], d_s, d_r, sp=peer(s, o, SP))
    second_group(half - 1)
    lagging()
    second_group(half)
    first = reduced(0)
    keys = first[:, C_LK:C_LV].astype(F32)
    values = first[:, C_LV:C_LQ].astype(F32)
    grow = jnp.exp(running)
    ends = jnp.where(ri < SPAN, end0, end1)
    ending = keys * jnp.exp(ends - running)
    state0 = over(values[:SPAN], ending[:SPAN], 0, 0, HIGH)
    state1 = state0 * jnp.exp(end1) + over(values[SPAN:], ending[SPAN:], 0, 0, HIGH)
    packed = state1.astype(BF16)
    st_send[...] = packed.reshape(SP, vr, LK)
    st_recv[s] = st_send[s]
    for o in range(1, SP):
        to = peer(s, o, SP)
        send(st_send.at[to], st_recv.at[s], st_s, st_r, sp=to)

    lagging()
    landed(1)
    project(1)
    project(2)
    lagging()
    arrived(dlog.at[pl.ds(0, SP - 1)], d_r)
    arrived(st_recv.at[pl.ds(0, SP - 1)], st_r)
    state = startt[pl.ds(pl.multiple_of(s * vr, vr), vr), :]
    for k in range(SP):
        pre_send[k] = state.astype(BF16)
        if k < SP - 1:
            state = state * jnp.exp(dlog[k][0:1, :]) + st_recv[k].astype(F32)
    pre_recv[s] = pre_send[s]
    for o in range(1, SP):
        to = peer(s, o, SP)
        send(pre_send.at[to], pre_recv.at[s], pre_s, pre_r, sp=to)
    lagging()
    kv[1] = reduced(1)
    send(kv.at[1], kv.at[0], kv_s, kv_r, sp=right)
    lagging()
    second = reduced(2)
    lagging()
    inverse = keys * jnp.exp(-running)
    query = second[:, :C_WQ - C_LQ].astype(F32) * (LK ** -0.5) * grow
    raws = []
    for n in range(2):
        span = slice(n * SPAN, (n + 1) * SPAN)
        inner = over(query[span], inverse[span], 1, 1, HIGH)
        inner = jnp.where(ri[:SPAN, :SPAN] >= ci[:SPAN, :SPAN], inner, 0.0)
        raws.append(over(inner, values[span], 1, 0, HIGH))
    raws[1] = raws[1] + over(query[SPAN:], state0, 1, 1, HIGH)
    arrived(kv.at[0], kv_r)
    kvs = jnp.concatenate([kv[0], kv[1]], axis=0)
    kw, vw = kvs[:, :HD], kvs[:, HD:]
    qi = lax.broadcasted_iota(jnp.int32, (TOK, 2 * TOK), 0)
    ki = lax.broadcasted_iota(jnp.int32, (TOK, 2 * TOK), 1)
    distance = qi - ki + TOK
    allowed = (distance >= 0) & (distance < TOK) & ((ki >= TOK) | (s > 0))
    far = distance.astype(F32)
    nears = []
    for h in range(HEADS):
        qh = second[:, C_WQ - C_LQ + h * HD:C_WQ - C_LQ + (h + 1) * HD]
        scores = over(qh, kw, 1, 1) * (HD ** -0.5)
        head = jnp.full((1, 1), t * HEADS + h + 1, jnp.int32).astype(F32)
        slope = jnp.exp2(-8.0 * head / (HEADS * TP))
        weights = jnp.where(allowed, jnp.exp(scores - slope * far), 0.0)
        total = jnp.sum(weights, axis=1, keepdims=True) + jnp.exp(sink_ref[0:1, h:h + 1])
        probs = (weights / total).astype(BF16)
        nears.append(over(probs, vw, 1, 0).astype(BF16))
    og[f, :, :HEADS * HD] = jnp.concatenate(nears, axis=1)

    def share(part_index):
        lanes = pl.ds(part_index * DV, DV)
        for o in range(1, FS):
            send(og.at[f, :, lanes], og.at[f, :, lanes], og_s, og_r.at[part_index, o - 1],
                 fs=peer(f, o, FS))

    share(0)
    while done[0] <= half:
        lagging()
    landed(2)
    landed(3)
    per = 128 // q
    for k in range(SP // per):
        for side in range(2):
            wcat[side * DV:(side + 1) * DV, k * 128:(k + 1) * 128] = jnp.concatenate(
                [wo[core, k * per + i][:, side * q:(side + 1) * q] for i in range(per)], axis=1
            )

    arrived(pre_recv.at[pl.ds(0, SP - 1)], pre_r)
    before = pre_recv[...].reshape(DV, LK).astype(F32)
    raws[0] = raws[0] + over(query[:SPAN], before, 1, 1, HIGH)
    raws[1] = raws[1] + over(query[SPAN:] * jnp.exp(end0), before, 1, 1, HIGH)
    raw = jnp.concatenate(raws, axis=0)
    gated = raw * lax.rsqrt(jnp.mean(raw * raw, axis=1, keepdims=True) + EPS) * lgain_ref[...]
    og[f, :, DV:] = gated.astype(BF16)
    share(1)
    order = [0] + sorted(range(1, FS), key=lambda o: min(o, FS - o))

    def chip_sum(o):
        arrived(pr_recv.at[o], pr_r.at[o])
        for e in range(X):
            to = peer(xi, e, X)
            both = po[o, to, core].astype(F32) + pr_recv[o, to].astype(F32)
            pr_send[o, e] = both.astype(BF16)
            if o > 0 or e > 0:
                send(pr_send.at[o, e], xr_recv.at[o, e], xr_s.at[min(o, 1)], xr_r.at[o],
                     tp=to * 2 + core, fs=peer(f, o, FS))

    for i, o in enumerate(order):
        source = peer(f, o, FS)
        if o > 0:
            for part_index in range(2):
                arrived(og.at[source, :, pl.ds(part_index * DV, DV)],
                        og_r.at[part_index, FS - 1 - o])
        po[o] = over(og[source], wcat[...], 1, 0).astype(BF16).reshape(X, 2, tr, SP * q)
        send(po.at[o, :, 1 - core], pr_recv.at[o], pr_s, pr_r.at[o], tp=twin)
        if i > 0:
            chip_sum(order[i - 1])
    chip_sum(order[-1])
    for o in order:
        if o > 0:
            arrived(xr_recv.at[o], xr_r.at[o])
            total = xr_recv[o, 0].astype(F32)
        else:
            if X > 1:
                arrived(xr_recv.at[o, pl.ds(1, X - 1)], xr_r.at[o])
            total = pr_send[o, 0].astype(F32)
        for e in range(1, X):
            total = total + xr_recv[o, e].astype(F32)
        fin[peer(f, FS - o, FS)] = total.astype(BF16)
    stored = []
    for side in range(2):
        for z in range(side * half, (side + 1) * half):
            out_ref[:, z * ROWS:(z + 1) * ROWS] = jnp.concatenate(
                [fin[k][:, z * q:(z + 1) * q] for k in range(FS)], axis=1
            )
        lanes = pl.ds(side * half * ROWS, half * ROWS)
        c = pltpu.make_async_copy(out_ref.at[:, lanes], out_hbm.at[:, lanes], out_s.at[side])
        c.start()
        stored.append(c)
    for group in range(4):
        @pl.when(carries(group))
        def _():
            left_here(many(group, both_cores), ring_s.at[group])
            left_here(many(group, 1 - carrier(group)), w_s.at[group])

        @pl.when(jnp.logical_not(carries(group)))
        def _():
            own_copy(group).wait_send()

    left_here(xs.at[pl.ds(0, FS - 1)], y_s)
    left_here(xg.at[:, :, pl.ds(0, X * ft)], x_s)
    if X > 1:
        left_here(xg.at[:, :, pl.ds(0, (X - 1) * ft)], xf_s)
        left_here(pr_send.at[0, pl.ds(1, X - 1)], xr_s.at[0])
    left_here(aux.at[pl.ds(0, TP - 1)], a_s)
    left_here(dlog.at[pl.ds(0, SP - 1)], d_s)
    left_here(rs_send, rs_s)
    left_here(kv.at[0], kv_s)
    left_here(st_send.at[pl.ds(0, SP - 1)], st_s)
    left_here(pre_send.at[pl.ds(0, SP - 1)], pre_s)
    left_here(og.at[pl.ds(0, FS - 1)], og_s)
    left_here(po.at[:, :, 0], pr_s)
    left_here(pr_send.at[pl.ds(1, FS - 1)], xr_s.at[1])
    for c in stored:
        c.wait()


def local(SP, FS, TP, *arrays):
    (activations, input_norm_gain, wq, wk, wv, lq, lk, lv, down, up, bias, extra, start, sink,
     lgain, wow, wol) = arrays
    q, ft, vr, tr = ROWS // FS, FEAT // FS, DV // SP, TOK // TP
    half = SP // 2
    dma = pltpu.SemaphoreType.DMA
    operands = (
        activations, input_norm_gain.reshape(-1, 128), wq, wk.T, wv.T, lq, lk, lv, down.T, up,
        bias.reshape(1, -1), extra.reshape(1, -1), start.reshape(LK, DV), sink.reshape(1, -1),
        lgain.reshape(1, -1), wow, wol,
    )
    held = [operands[i] for i in (0, 1, 3, 4, 8, 9, 10, 11, 12, 13, 14, 15, 16)]
    X = TP // 2
    return pl.pallas_call(
        functools.partial(kernel, SP, FS, TP),
        out_shape=jax.ShapeDtypeStruct((tr, SP * ROWS), BF16),
        in_specs=[pl.BlockSpec(memory_space=pl.ANY)] * len(operands),
        out_specs=pl.BlockSpec(memory_space=pl.ANY),
        scratch_shapes=[pltpu.VMEM((tr, SP * ROWS), BF16)] + [pltpu.VMEM(a.shape, a.dtype) for a in held] + [
            pltpu.VMEM((FS, TOK, ft), BF16),
            pltpu.VMEM((FS, TOK, TP * ft), BF16),
            pltpu.VMEM((TP, RANK + 8, TOK), F32),
            pltpu.VMEM((2, SP * q, C_END), BF16),
            pltpu.VMEM((2, SP, 256, 2 * q), BF16),
            pltpu.VMEM((2 * DV, SP * q), BF16),
            pltpu.VMEM((FS - 1, TOK, C_END), BF16),
            pltpu.VMEM((FS - 1, TOK, C_END), BF16),
            pltpu.VMEM((2, TOK, 2 * HD), BF16),
            pltpu.VMEM((SP, vr, LK), BF16),
            pltpu.VMEM((SP, vr, LK), BF16),
            pltpu.VMEM((SP, 8, LK), F32),
            pltpu.VMEM((SP, vr, LK), BF16),
            pltpu.VMEM((SP, vr, LK), BF16),
            pltpu.VMEM((DV, LK), F32),
            pltpu.VMEM((FS, TOK, 2 * DV), BF16),
            pltpu.VMEM((FS, X, 2, tr, SP * q), BF16),
            pltpu.VMEM((FS, X, tr, SP * q), BF16),
            pltpu.VMEM((FS, X, tr, SP * q), BF16),
            pltpu.VMEM((FS, X, tr, SP * q), BF16),
            pltpu.VMEM((FS, tr, SP * q), BF16),
            dma((len(operands),)), dma((2,)),
            dma((4,)), dma((4,)),
            dma((4,)), dma((4,)),
            dma((4,)), dma((6, 2, half)),
            dma, dma,
            dma, dma((X,)),
            dma, dma,
            dma, dma,
            dma, dma,
            dma, dma((3,)),
            dma, dma,
            dma, dma,
            dma, dma,
            dma, dma((2, FS - 1)),
            dma, dma((FS,)),
            dma((2,)), dma((FS,)),
            dma, dma,
        ],
        compiler_params=pltpu.CompilerParams(
            collective_id=0, has_side_effects=True, vmem_limit_bytes=60 * 1024 * 1024
        ),
    )(*operands)


def solution(mesh):
    placed = (
        P(("fs", "sp"), "tp"), P(), P("sp", "tp"), P("sp", "tp"), P("sp", "tp"), P("sp", "tp"),
        P("sp", "tp"), P("sp", "tp"), P(), P(None, "tp"), P("tp"), P(("fs", "sp"), "tp"),
        P("tp", None, None), P("tp"), P(), P("tp", "sp"), P("tp", "sp"),
    )
    sizes = (mesh.shape["sp"], mesh.shape["fs"], mesh.shape["tp"])
    return jax.shard_map(
        functools.partial(local, *sizes), mesh=mesh, in_specs=placed,
        out_specs=P(("fs", "sp", "tp"), None), check_vma=False,
    )
```
